32 devices in a mesh: sp: 8 (over z, y), tp: 4 (over x, core).
Axes of the slice: x: 2, y: 2, z: 4, core: 2. Of those that a mesh axis runs over, the one named last changes fastest.
Arguments:
- residual: bfloat16 [3072, 2048], P(('sp', 'tp')), may hold values from -6 to 6
- query_logits: bfloat16 [3072, 2048], P('sp', 'tp'), may hold values from -6 to 6
- value_written: bfloat16 [3072, 2048], P('sp', 'tp'), may hold values from -6 to 6
- output_gate_logits: bfloat16 [3072, 2048], P('sp', 'tp'), may hold values from -6 to 6
- forget_logits: bfloat16 [2, 3072, 2048], P(None, 'sp', 'tp'), may hold values from -6 to 6
- forget_slack: float32 [2, 2048], P(None, 'tp'), may hold values from 0 to 0.06, as said below
- spike_log_decay: float32 [16, 3072], P('tp', 'sp'), may hold values from -1.4 to 0
- head_norm_scale: float32 [128], replicated, may hold values from 0.1 to 1.9
- recurrence_output_matrix: bfloat16 [2048, 2048], replicated, may hold values from -0.125 to 0.125
- feed_norm_scale: float32 [2048], replicated, may hold values from 0.1 to 1.9
- gate_matrix: bfloat16 [2048, 5120], P('sp', 'tp'), may hold values from -0.125 to 0.125
- up_matrix: bfloat16 [2048, 5120], P('sp', 'tp'), may hold values from -0.125 to 0.125
- position_filter_taps: float32 [2, 3, 5120], P(None, None, 'tp'), may hold values from -3.5 to 3.5
- down_matrix: bfloat16 [5120, 2048], P('tp', 'sp'), may hold values from -0.078125 to 0.078125
Outputs:
- layer_out: bfloat16 [3072, 2048], P(('sp', 'tp'))
The draws below stay inside these ranges and needn't reach their ends.
Inputs may be any that keep to these rules, and one draw needn't show every extreme that they name: `forget_slack`: every entry is positive.
All inputs are finite; a program needn't handle non-finite values.
Results may differ from the reference program's by a relative error of at most 0.015.
Values may be sent and summed in bfloat16 or wider, within the bound.
A program may use at most 64 MiB of HBM per device.

```python
import math
import jax
import jax.numpy as jnp
from jax import lax

HEADS = 16
HEAD = 128
D = 2048
FF = 5120
TOK_DEV = 384
TOKENS = 3072
N_TP = 4


def draw_forget_logits(key, part):
    noise_key = jax.random.fold_in(key, 11)
    block_key = jax.random.fold_in(key, 12)
    lasting_key = jax.random.fold_in(key, 13)
    noise = jnp.clip(jax.random.normal(noise_key, (2, TOKENS, D), jnp.float32), -3.0, 3.0)
    block_shifts = jax.random.uniform(block_key, (2, TOKENS // TOK_DEV, D), jnp.float32, -2.5, 2.5)
    lasting_shifts = jax.random.uniform(lasting_key, (2, 1, D), jnp.float32, -2.0, 2.0)
    summed = noise + jnp.repeat(block_shifts, TOK_DEV, axis=1) + lasting_shifts
    return jnp.clip(summed, -6.0, 6.0).astype(jnp.bfloat16)


def draw_forget_slack(key, part):
    slow_share = 0.5
    slow_heads = jax.random.uniform(jax.random.fold_in(key, 21), (1, HEADS, 1), jnp.float32) < slow_share
    slow_rate = jnp.exp(jax.random.uniform(jax.random.fold_in(key, 22), (2, HEADS, HEAD), jnp.float32, math.log(0.25), math.log(4.0))) / TOKENS
    fast_rate = jnp.exp(jax.random.uniform(jax.random.fold_in(key, 23), (2, HEADS, HEAD), jnp.float32, math.log(0.02), math.log(0.06)))
    return jnp.where(slow_heads, slow_rate, fast_rate).reshape(2, D).astype(jnp.float32)


def draw_spike_log_decay(key, part):
    places = jax.random.randint(jax.random.fold_in(key, 31), (HEADS, 2, 1), 0, TOKENS)
    depths = jnp.log(jax.random.uniform(jax.random.fold_in(key, 32), (HEADS, 2, 1), jnp.float32, 0.5, 0.8))
    hits = jnp.arange(TOKENS, dtype=jnp.int32)[None, None, :] == places
    return jnp.sum(jnp.where(hits, depths, 0.0), axis=1).astype(jnp.float32)


def block_levels(stream_key, extent, cuts, low, largest):
    factor_of = 1.0
    for position, parts in cuts:
        steps = jax.random.uniform(jax.random.fold_in(jax.random.fold_in(stream_key, 6), position), (parts,), jnp.float32, low / len(cuts), largest / len(cuts))
        factor_of = factor_of * jnp.repeat(jnp.exp(steps), extent[position] // parts).reshape((-1,) + (1,) * (len(extent) - 1 - position))
    return factor_of


def normal_values(rng, dims, spread, limit, split=(), kind=jnp.bfloat16):
    loudness = block_levels(rng, dims, split, -0.22, 0.18) if split else 1.0
    values = jax.random.normal(rng, dims, jnp.float32) * spread * loudness
    return jnp.minimum(jnp.maximum(values, -limit), limit).astype(kind)


def setup_inputs(seed: int = 0) -> dict:
    key_list = jax.random.split(jax.random.key(seed), 15)
    return {
        "residual": normal_values(key_list[0], (TOKENS, D), 1.0, 6.0, ((0, 32),)),
        "query_logits": normal_values(key_list[1], (TOKENS, D), 1.0, 6.0, ((0, 8), (1, 4))),
        "value_written": normal_values(key_list[2], (TOKENS, D), 1.0, 6.0, ((0, 8), (1, 4))),
        "output_gate_logits": normal_values(key_list[3], (TOKENS, D), 1.0, 6.0, ((0, 8), (1, 4))),
        "forget_logits": draw_forget_logits(jax.random.fold_in(key_list[14], 71), 0),
        "forget_slack": draw_forget_slack(jax.random.fold_in(key_list[14], 71), 0),
        "spike_log_decay": draw_spike_log_decay(jax.random.fold_in(key_list[14], 71), 0),
        "head_norm_scale": jnp.clip(1.0 + 0.18 * jax.random.normal(key_list[7], (HEAD,), jnp.float32), 0.1, 1.9),
        "recurrence_output_matrix": normal_values(key_list[8], (D, D), D ** -0.5, 0.125),
        "feed_norm_scale": jnp.clip(1.0 + 0.18 * jax.random.normal(key_list[9], (D,), jnp.float32), 0.1, 1.9),
        "gate_matrix": normal_values(key_list[10], (D, FF), D ** -0.5, 0.125, ((0, 8), (1, 4))),
        "up_matrix": normal_values(key_list[11], (D, FF), D ** -0.5, 0.125, ((0, 8), (1, 4))),
        "position_filter_taps": normal_values(key_list[12], (2, 3, FF), 3 ** -0.5, 3.5, ((2, 4),), jnp.float32),
        "down_matrix": normal_values(key_list[13], (FF, D), FF ** -0.5, 0.078125, ((0, 4), (1, 8))),
    }


PRECISE = lax.Precision.HIGHEST
EPSILON = 1e-06

def run_blocks(queries, key_in, values, log_keep):
    head_count, length, per_head_width = queries.shape
    block_len = math.gcd(length, 64)
    block_count = length // block_len

    def to_blocks(tensor):
        return jnp.swapaxes(tensor.reshape(head_count, block_count, block_len, tensor.shape[-1]), 0, 1)
    lower_mask = jnp.tril(jnp.ones((block_len, block_len), jnp.float32))

    def advance(carried, pieces):
        query_block, key_block, value_block, keep_block = pieces
        running = jnp.cumsum(keep_block, axis=1)
        ending = running[:, -1:, :]
        query_scaled = query_block * jnp.exp(running)
        scores = jnp.einsum('hsd,htd->hst', query_scaled, key_block * jnp.exp(-running), precision=PRECISE) * lower_mask
        result = jnp.einsum('hst,htv->hsv', scores, value_block, precision=PRECISE)
        result = result + jnp.einsum('hsd,hdv->hsv', query_scaled, carried, precision=PRECISE)
        fresh_state = jnp.einsum('htd,htv->hdv', key_block * jnp.exp(ending - running), value_block, precision=PRECISE)
        return (jnp.exp(ending[:, 0, :])[:, :, None] * carried + fresh_state, result)
    initial = jnp.zeros((head_count, per_head_width, values.shape[-1]), jnp.float32)
    last_state, outputs = lax.scan(advance, initial, (to_blocks(queries), to_blocks(key_in), to_blocks(values), to_blocks(log_keep)))
    return (jnp.swapaxes(outputs, 0, 1).reshape(head_count, length, values.shape[-1]), last_state)

def to_heads(block, per_head_width):
    row_count = block.shape[0]
    return jnp.swapaxes(block.reshape(row_count, -1, per_head_width), 0, 1).astype(jnp.float32)

def reverse_rows(tensor):
    return jnp.flip(tensor, axis=1)

def build_inputs(forget_gate_rows, forget_slack_row, spike_decay_rows, per_head_width):
    leak_heads = forget_slack_row.reshape(-1, per_head_width)[:, None, :]
    key_direction = leak_heads * jax.nn.sigmoid(-to_heads(forget_gate_rows, per_head_width))
    return (key_direction, jnp.log1p(-key_direction) + spike_decay_rows)

def gate_heads(summed, head_norm_scale, output_gate_logits):
    scaled = summed * lax.rsqrt(lax.optimization_barrier(jnp.mean(summed * summed, axis=-1, keepdims=True)) + EPSILON) * head_norm_scale
    flattened = jnp.swapaxes(scaled, 0, 1).reshape(summed.shape[1], -1)
    return (flattened * jax.nn.silu(output_gate_logits.astype(jnp.float32))).astype(jnp.bfloat16)

def rms_scale(layer_state, feed_norm_scale):
    widened = layer_state.astype(jnp.float32)
    return (widened * lax.rsqrt(lax.optimization_barrier(jnp.mean(widened * widened, axis=-1, keepdims=True)) + EPSILON) * feed_norm_scale).astype(jnp.bfloat16)

def conv_gate(padded, tap_rows):
    length = padded.shape[0] - 2
    mixed_rows = tap_rows[0] * padded[0:length] + tap_rows[1] * padded[1:length + 1] + tap_rows[2] * padded[2:length + 2]
    half_width = mixed_rows.shape[1] // 2
    return (jax.nn.silu(mixed_rows[:, :half_width]) * mixed_rows[:, half_width:]).astype(jnp.bfloat16)

def reference(residual, query_logits, value_written, output_gate_logits, forget_logits, forget_slack, spike_log_decay, head_norm_scale, recurrence_output_matrix, feed_norm_scale, gate_matrix, up_matrix, position_filter_taps, down_matrix):
    per_head_width = head_norm_scale.shape[0]
    queries = jax.nn.silu(to_heads(query_logits, per_head_width))
    values = to_heads(value_written, per_head_width)
    spike_decay_rows = spike_log_decay[:, :, None]
    key_forward, retain_forward = build_inputs(forget_logits[0], forget_slack[0], spike_decay_rows, per_head_width)
    key_backward, retain_backward = build_inputs(forget_logits[1], forget_slack[1], spike_decay_rows, per_head_width)
    out_fwd = run_blocks(queries, key_forward, values, retain_forward)[0]
    out_bwd = run_blocks(reverse_rows(queries), reverse_rows(key_backward), reverse_rows(values), reverse_rows(retain_backward))[0]
    gated_heads = gate_heads(out_fwd + reverse_rows(out_bwd), head_norm_scale, output_gate_logits)
    branch = jnp.dot(gated_heads, recurrence_output_matrix, preferred_element_type=jnp.float32)
    layer_state = (residual.astype(jnp.float32) + branch).astype(jnp.bfloat16)
    normed = rms_scale(layer_state, feed_norm_scale)
    gate_proj = jnp.dot(normed, gate_matrix, preferred_element_type=jnp.float32).astype(jnp.bfloat16)
    up_proj = jnp.dot(normed, up_matrix, preferred_element_type=jnp.float32).astype(jnp.bfloat16)
    projected = jnp.concatenate([gate_proj, up_proj], axis=1)
    padded = jnp.pad(projected, ((1, 1), (0, 0)))
    tap_rows = jnp.concatenate([position_filter_taps[0], position_filter_taps[1]], axis=1)
    hidden = conv_gate(padded, tap_rows)
    group_width = hidden.shape[1] // N_TP

    def add_group(running_sum, group_index):
        partial_value = jnp.dot(lax.dynamic_slice_in_dim(hidden, group_index * group_width, group_width, 1), lax.dynamic_slice_in_dim(down_matrix, group_index * group_width, group_width, 0), preferred_element_type=jnp.float32)
        rounded = lax.optimization_barrier(partial_value.astype(jnp.bfloat16))
        return (running_sum + rounded.astype(jnp.float32), None)
    channel_out = lax.scan(add_group, jnp.zeros((hidden.shape[0], down_matrix.shape[1]), jnp.float32), jnp.arange(N_TP, dtype=jnp.int32))[0]
    return (layer_state.astype(jnp.float32) + channel_out).astype(jnp.bfloat16)
```

```python
import jax
import jax.numpy as jnp
from jax import lax
from jax.sharding import PartitionSpec as P

PRECISE = lax.Precision.HIGHEST
EPSILON = 1e-06


def extended(block, sides, width):
    for axis, dim in sides:
        count = lax.axis_size(axis)
        forward = [(i, i + 1) for i in range(count - 1)]
        backward = [(target, source) for source, target in forward]
        low = lax.ppermute(
            lax.slice_in_dim(block, block.shape[dim] - width, None, axis=dim), axis, forward
        )
        high = lax.ppermute(lax.slice_in_dim(block, 0, width, axis=dim), axis, backward)
        block = jnp.concatenate([low, block, high], axis=dim)
    return block


def bf(tensor):
    return tensor.astype(jnp.bfloat16)


def mm(left, right, dims=((1,), (0,))):
    return lax.dot_general(bf(left), bf(right), (dims, ((), ())), preferred_element_type=jnp.float32)


def split_sum(mask, terms):
    high = bf(terms)
    low = bf(terms - high.astype(jnp.float32))
    return mm(mask, high) + mm(mask, low)


def direction(queries, logits, slack, causal, spike_col, spike_row, last):
    keys = slack * jax.nn.sigmoid(-logits)
    running = split_sum(causal, jnp.log1p(-keys))
    ending = running[last : last + 1] if last >= 0 else running[-1:]
    spike_end = spike_col[last : last + 1] if last >= 0 else spike_col[-1:]
    rising = jnp.exp(running)
    scores = mm(queries * rising, keys * jnp.exp(-running), ((1,), (1,)))
    factor = jnp.exp(jnp.where(causal > 0, spike_col - spike_row, -1e30))
    to_state = keys * jnp.exp((ending - running) + (spike_end - spike_col))
    entering = queries * (rising * jnp.exp(spike_col))
    return scores * factor, to_state, entering, ending + spike_end


def gate_head(summed, head_norm_scale, output_gate_logits):
    scaled = (
        summed
        * lax.rsqrt(jnp.mean(summed * summed, axis=-1, keepdims=True) + EPSILON)
        * head_norm_scale
    )
    return bf(scaled * jax.nn.silu(output_gate_logits.astype(jnp.float32)))


def rms_scale(layer_state, feed_norm_scale):
    widened = layer_state.astype(jnp.float32)
    return (
        widened
        * lax.rsqrt(jnp.mean(widened * widened, axis=-1, keepdims=True) + EPSILON)
        * feed_norm_scale
    ).astype(jnp.bfloat16)


def conv_gate(padded, tap_rows):
    length = padded.shape[0] - 2
    mixed_rows = (
        tap_rows[0] * padded[0:length]
        + tap_rows[1] * padded[1 : length + 1]
        + tap_rows[2] * padded[2 : length + 2]
    )
    half_width = mixed_rows.shape[1] // 2
    return (jax.nn.silu(mixed_rows[:, :half_width]) * mixed_rows[:, half_width:]).astype(
        jnp.bfloat16
    )


def entering_states(states, decays, reverse):
    count, index = decays.shape[0], lax.axis_index("sp")
    place = jnp.arange(count)
    order = place[:, None] < place[None, :]
    if reverse:
        between = (place[None, :] < place[:, None]) & (place[None, :] > index)
        used = place > index
    else:
        between = (place[None, :] > place[:, None]) & (place[None, :] < index)
        used = place < index
    total = jnp.einsum(
        "jm,mhd->jhd", between.astype(jnp.float32), decays, precision=PRECISE
    )
    weight = jnp.exp(total) * used[:, None, None]
    return jnp.sum(weight[:, :, :, None] * states.astype(jnp.float32), axis=0)


def on_device(
    residual,
    query_logits,
    value_written,
    output_gate_logits,
    forget_logits,
    forget_slack,
    spike_log_decay,
    head_norm_scale,
    recurrence_output_matrix,
    feed_norm_scale,
    gate_matrix,
    up_matrix,
    position_filter_taps,
    down_matrix,
):
    gate_all, up_all, down_all = (
        lax.all_gather(gate_matrix, "sp", axis=0, tiled=True),
        lax.all_gather(up_matrix, "sp", axis=0, tiled=True),
        lax.all_gather(down_matrix, "sp", axis=1, tiled=True),
    )
    width = head_norm_scale.shape[0]
    length, columns = query_logits.shape
    place = jnp.arange(length)
    lower = (place[:, None] >= place[None, :]).astype(jnp.float32)
    upper = lower.T
    spike_rows = jnp.stack(
        [
            jnp.dot(spike_log_decay, upper, precision=PRECISE),
            jnp.dot(spike_log_decay, lower, precision=PRECISE),
        ]
    )
    within, states, entering, decays = [], [], [], []
    for head in range(columns // width):
        cut = slice(head * width, (head + 1) * width)
        queries = jax.nn.silu(query_logits[:, cut].astype(jnp.float32))
        pieces = [
            direction(
                queries,
                forget_logits[way][:, cut].astype(jnp.float32),
                forget_slack[way : way + 1, cut],
                (lower, upper)[way],
                spike_rows[way, head][:, None],
                spike_rows[way, head][None, :],
                (-1, 0)[way],
            )
            for way in range(2)
        ]
        within.append(mm(pieces[0][0] + pieces[1][0], value_written[:, cut]))
        states.append([bf(mm(p[1], value_written[:, cut], ((0,), (0,)))) for p in pieces])
        entering.append(bf(jnp.concatenate([p[2] for p in pieces], axis=1)))
        decays.append(jnp.concatenate([p[3] for p in pieces], axis=0))
    decays = lax.all_gather(jnp.stack(decays), "sp")
    enters = []
    for way in range(2):
        mine = [s[way] for s in states]
        parts = [
            lax.all_gather(jnp.stack(part), "sp") for part in (mine[: len(mine) // 2], mine[len(mine) // 2 :])
        ]
        enters.append(
            entering_states(jnp.concatenate(parts, axis=1), decays[:, :, way], way == 1)
        )
    gated = []
    for head in range(columns // width):
        cut = slice(head * width, (head + 1) * width)
        state = jnp.concatenate([enters[0][head], enters[1][head]], axis=0)
        summed = within[head] + mm(entering[head], state)
        gated.append(gate_head(summed, head_norm_scale, output_gate_logits[:, cut]))
    gated_heads = jnp.concatenate(gated, axis=1)
    regrouped = lax.all_to_all(gated_heads, "tp", split_axis=0, concat_axis=1, tiled=True)
    branch = jnp.dot(regrouped, recurrence_output_matrix, preferred_element_type=jnp.float32)
    layer_state = (residual.astype(jnp.float32) + branch).astype(jnp.bfloat16)
    normed = rms_scale(layer_state, feed_norm_scale)
    half = normed.shape[1] // 2
    row_piece = jnp.concatenate(
        [
            lax.all_gather(normed[:, :half], "tp", axis=0, tiled=True),
            lax.all_gather(normed[:, half:], "tp", axis=0, tiled=True),
        ],
        axis=1,
    )
    gate_part = jnp.dot(row_piece, gate_all, preferred_element_type=jnp.float32)
    up_part = jnp.dot(row_piece, up_all, preferred_element_type=jnp.float32)
    projected = jnp.concatenate([gate_part, up_part], axis=1).astype(jnp.bfloat16)
    padded = extended(projected, (("sp", 0),), 1)
    tap_rows = jnp.concatenate([position_filter_taps[0], position_filter_taps[1]], axis=1)
    hidden = conv_gate(padded, tap_rows)
    channel_out = lax.psum_scatter(
        jnp.dot(hidden, down_all, preferred_element_type=jnp.float32).astype(jnp.bfloat16),
        "tp",
        scatter_dimension=0,
        tiled=True,
    ).astype(jnp.float32)
    return (layer_state.astype(jnp.float32) + channel_out).astype(jnp.bfloat16)


def solution(mesh):
    placed = (
        P(("sp", "tp"), None),
        P("sp", "tp"),
        P("sp", "tp"),
        P("sp", "tp"),
        P(None, "sp", "tp"),
        P(None, "tp"),
        P("tp", "sp"),
        P(),
        P(),
        P(),
        P("sp", "tp"),
        P("sp", "tp"),
        P(None, None, "tp"),
        P("tp", "sp"),
    )
    return jax.shard_map(
        on_device, mesh=mesh, in_specs=placed, out_specs=P(("sp", "tp"), None), check_vma=False
    )
```

```python
import functools

import jax
import jax.numpy as jnp
from jax import lax
from jax.sharding import PartitionSpec as P

PRECISE = lax.Precision.HIGHEST
EPSILON = 1e-06


def extended(block, sides, width):
    for axis, dim in sides:
        count = lax.axis_size(axis)
        forward = [(i, i + 1) for i in range(count - 1)]
        backward = [(target, source) for source, target in forward]
        low = lax.ppermute(
            lax.slice_in_dim(block, block.shape[dim] - width, None, axis=dim), axis, forward
        )
        high = lax.ppermute(lax.slice_in_dim(block, 0, width, axis=dim), axis, backward)
        block = jnp.concatenate([low, block, high], axis=dim)
    return block


def bf(tensor):
    return tensor.astype(jnp.bfloat16)


def mm(left, right, dims=((1,), (0,))):
    return lax.dot_general(bf(left), bf(right), (dims, ((), ())), preferred_element_type=jnp.float32)


def split_sum(mask, terms):
    high = bf(terms)
    low = bf(terms - high.astype(jnp.float32))
    return mm(mask, high) + mm(mask, low)


def direction(queries, logits, slack, causal, spike_col, spike_row, last):
    keys = slack * jax.nn.sigmoid(-logits)
    running = split_sum(causal, jnp.log1p(-keys))
    ending = running[last : last + 1] if last >= 0 else running[-1:]
    spike_end = spike_col[last : last + 1] if last >= 0 else spike_col[-1:]
    rising = jnp.exp(running)
    scores = mm(queries * rising, keys * jnp.exp(-running), ((1,), (1,)))
    factor = jnp.exp(jnp.where(causal > 0, spike_col - spike_row, -1e30))
    to_state = keys * jnp.exp((ending - running) + (spike_end - spike_col))
    entering = queries * (rising * jnp.exp(spike_col))
    return scores * factor, to_state, entering, ending + spike_end


def gate_head(summed, head_norm_scale, output_gate_logits):
    scaled = (
        summed
        * lax.rsqrt(jnp.mean(summed * summed, axis=-1, keepdims=True) + EPSILON)
        * head_norm_scale
    )
    return bf(scaled * jax.nn.silu(output_gate_logits.astype(jnp.float32)))


def rms_scale(layer_state, feed_norm_scale):
    widened = layer_state.astype(jnp.float32)
    return (
        widened
        * lax.rsqrt(jnp.mean(widened * widened, axis=-1, keepdims=True) + EPSILON)
        * feed_norm_scale
    ).astype(jnp.bfloat16)


def conv_gate(padded, tap_rows):
    length = padded.shape[0] - 2
    mixed_rows = (
        tap_rows[0] * padded[0:length]
        + tap_rows[1] * padded[1 : length + 1]
        + tap_rows[2] * padded[2 : length + 2]
    )
    half_width = mixed_rows.shape[1] // 2
    return (jax.nn.silu(mixed_rows[:, :half_width]) * mixed_rows[:, half_width:]).astype(
        jnp.bfloat16
    )


def ring_order(mesh):
    count = mesh.shape["sp"]
    places = [getattr(d, "coords", None) for d in mesh.devices.reshape(count, -1)[:, 0]]
    if any(p is None for p in places):
        return list(range(count))
    at = {(p[2], p[1]): index for index, p in enumerate(places)}
    tall = 1 + max(z for z, _ in at)
    wide = 1 + max(y for _, y in at)
    if len(at) != count or tall * wide != count or tall % 2 or wide < 2:
        return list(range(count))
    walk = []
    for z in range(tall):
        ys = range(1, wide) if z % 2 == 0 else range(wide - 1, 0, -1)
        walk += [(z, y) for y in ys]
    walk += [(z, 0) for z in range(tall - 1, -1, -1)]
    return [at[p] for p in walk]


def ring_gather(block, order, step_sign):
    count = len(order)
    pairs = [(order[p], order[(p + step_sign) % count]) for p in range(count)]
    position = [order.index(index) for index in range(count)]
    me = lax.axis_index("sp")
    arrived = [(block, me)]
    for step in range(1, count):
        block = lax.ppermute(block, "sp", pairs)
        owners = [order[(position[index] - step_sign * step) % count] for index in range(count)]
        arrived.append((block, jnp.array(owners, jnp.int32)[me]))
    return arrived


def assemble(arrived, axis):
    block = arrived[0][0]
    shape = list(block.shape)
    extent = shape[axis]
    shape[axis] *= len(arrived)
    whole = jnp.zeros(shape, block.dtype)
    for piece, owner in arrived:
        whole = lax.dynamic_update_slice_in_dim(whole, piece, owner * extent, axis)
    return whole


def entering_states(forward, backward):
    count, me = lax.axis_size("sp"), lax.axis_index("sp")
    received = {}
    for k in range(1, count):
        outgoing = jnp.where(me + k < count, forward, backward)
        received[k] = lax.ppermute(outgoing, "sp", [(p, (p + k) % count) for p in range(count)])
    width = forward.shape[2]
    totals = []
    for ks, later in ((range(1, count), False), (range(count - 1, 0, -1), True)):
        total = jnp.zeros(forward[:, :width].shape, jnp.float32)
        scale = jnp.ones((forward.shape[0], width), jnp.float32)
        for k in ks:
            used = (me - k < 0) if later else (me - k >= 0)
            state = received[k][:, :width].astype(jnp.float32)
            total = total + jnp.where(used, scale, 0.0)[:, :, None] * state
            scale = scale * received[k][:, width].astype(jnp.float32)
        totals.append(total)
    return totals


def on_device(
    order,
    residual,
    query_logits,
    value_written,
    output_gate_logits,
    forget_logits,
    forget_slack,
    spike_log_decay,
    head_norm_scale,
    recurrence_output_matrix,
    feed_norm_scale,
    gate_matrix,
    up_matrix,
    position_filter_taps,
    down_matrix,
):
    halves = down_matrix.shape[0] // 2
    gate_all = assemble(ring_gather(gate_matrix, order, 1), 0)
    up_all = assemble(ring_gather(up_matrix, order, -1), 0)
    down_parts = (
        assemble(ring_gather(down_matrix[:halves], order, 1), 1),
        assemble(ring_gather(down_matrix[halves:], order, -1), 1),
    )
    width = head_norm_scale.shape[0]
    length, columns = query_logits.shape
    place = jnp.arange(length)
    lower = (place[:, None] >= place[None, :]).astype(jnp.float32)
    upper = lower.T
    spike_rows = jnp.stack(
        [
            jnp.dot(spike_log_decay, upper, precision=PRECISE),
            jnp.dot(spike_log_decay, lower, precision=PRECISE),
        ]
    )
    within, states, entering, decays = [], [], [], []
    for head in range(columns // width):
        cut = slice(head * width, (head + 1) * width)
        queries = jax.nn.silu(query_logits[:, cut].astype(jnp.float32))
        pieces = [
            direction(
                queries,
                forget_logits[way][:, cut].astype(jnp.float32),
                forget_slack[way : way + 1, cut],
                (lower, upper)[way],
                spike_rows[way, head][:, None],
                spike_rows[way, head][None, :],
                (-1, 0)[way],
            )
            for way in range(2)
        ]
        within.append(mm(pieces[0][0] + pieces[1][0], value_written[:, cut]))
        states.append([bf(mm(p[1], value_written[:, cut], ((0,), (0,)))) for p in pieces])
        entering.append(bf(jnp.concatenate([p[2] for p in pieces], axis=1)))
        decays.append([p[3][0] for p in pieces])
    carried = []
    for way in range(2):
        state = jnp.stack([pair[way] for pair in states])
        decay = bf(jnp.exp(jnp.stack([pair[way] for pair in decays])))
        rows = jnp.broadcast_to(decay[:, None, :], (decay.shape[0], 16, width))
        carried.append(jnp.concatenate([state, rows], axis=1))
    enters = entering_states(*carried)
    gated = []
    for head in range(columns // width):
        cut = slice(head * width, (head + 1) * width)
        state = jnp.concatenate([enters[0][head], enters[1][head]], axis=0)
        summed = within[head] + mm(entering[head], state)
        gated.append(gate_head(summed, head_norm_scale, output_gate_logits[:, cut]))
    gated_heads = jnp.concatenate(gated, axis=1)
    regrouped = lax.all_to_all(gated_heads, "tp", split_axis=0, concat_axis=1, tiled=True)
    branch = jnp.dot(regrouped, recurrence_output_matrix, preferred_element_type=jnp.float32)
    layer_state = (residual.astype(jnp.float32) + branch).astype(jnp.bfloat16)
    normed = rms_scale(layer_state, feed_norm_scale)
    half = normed.shape[1] // 2
    row_piece = jnp.concatenate(
        [
            lax.all_gather(normed[:, :half], "tp", axis=0, tiled=True),
            lax.all_gather(normed[:, half:], "tp", axis=0, tiled=True),
        ],
        axis=1,
    )
    gate_part = jnp.dot(row_piece, gate_all, preferred_element_type=jnp.float32)
    up_part = jnp.dot(row_piece, up_all, preferred_element_type=jnp.float32)
    projected = jnp.concatenate([gate_part, up_part], axis=1).astype(jnp.bfloat16)
    padded = extended(projected, (("sp", 0),), 1)
    tap_rows = jnp.concatenate([position_filter_taps[0], position_filter_taps[1]], axis=1)
    hidden = conv_gate(padded, tap_rows)
    partial = jnp.dot(
        hidden[:, :halves], down_parts[0], preferred_element_type=jnp.float32
    ) + jnp.dot(hidden[:, halves:], down_parts[1], preferred_element_type=jnp.float32)
    groups = lax.axis_size("tp")
    sent = bf(partial).reshape(groups, -1, partial.shape[1])
    channel_out = jnp.sum(
        lax.all_to_all(sent, "tp", split_axis=0, concat_axis=0).astype(jnp.float32), axis=0
    )
    return (layer_state.astype(jnp.float32) + channel_out).astype(jnp.bfloat16)


def solution(mesh):
    placed = (
        P(("sp", "tp"), None),
        P("sp", "tp"),
        P("sp", "tp"),
        P("sp", "tp"),
        P(None, "sp", "tp"),
        P(None, "tp"),
        P("tp", "sp"),
        P(),
        P(),
        P(),
        P("sp", "tp"),
        P("sp", "tp"),
        P(None, None, "tp"),
        P("tp", "sp"),
    )
    return jax.shard_map(
        functools.partial(on_device, ring_order(mesh)),
        mesh=mesh,
        in_specs=placed,
        out_specs=P(("sp", "tp"), None),
        check_vma=False,
    )
```

```python
import jax
import jax.numpy as jnp
from jax import lax
from jax.sharding import PartitionSpec as P


PRECISE = lax.Precision.HIGHEST
EPSILON = 1e-06


def extended(block, sides, width):
    for axis, dim in sides:
        count = lax.axis_size(axis)
        forward = [(i, i + 1) for i in range(count - 1)]
        backward = [(target, source) for source, target in forward]
        low = lax.ppermute(
            lax.slice_in_dim(block, block.shape[dim] - width, None, axis=dim), axis, forward
        )
        high = lax.ppermute(lax.slice_in_dim(block, 0, width, axis=dim), axis, backward)
        block = jnp.concatenate([low, block, high], axis=dim)
    return block


def bf(tensor):
    return tensor.astype(jnp.bfloat16)


def mm(left, right, dims=((1,), (0,))):
    return lax.dot_general(bf(left), bf(right), (dims, ((), ())), preferred_element_type=jnp.float32)


def split_sum(mask, terms):
    high = bf(terms)
    low = bf(terms - high.astype(jnp.float32))
    return mm(mask, high) + mm(mask, low)


def direction(queries, logits, slack, causal, spike_col, spike_row, last):
    keys = slack * jax.nn.sigmoid(-logits)
    running = split_sum(causal, jnp.log1p(-keys))
    ending = running[last : last + 1] if last >= 0 else running[-1:]
    spike_end = spike_col[last : last + 1] if last >= 0 else spike_col[-1:]
    rising = jnp.exp(running)
    scores = mm(queries * rising, keys * jnp.exp(-running), ((1,), (1,)))
    factor = jnp.exp(jnp.where(causal > 0, spike_col - spike_row, -1e30))
    to_state = keys * jnp.exp((ending - running) + (spike_end - spike_col))
    entering = queries * (rising * jnp.exp(spike_col))
    return scores * factor, to_state, entering, ending + spike_end


def gate_head(summed, head_norm_scale, output_gate_logits):
    scaled = (
        summed
        * lax.rsqrt(jnp.mean(summed * summed, axis=-1, keepdims=True) + EPSILON)
        * head_norm_scale
    )
    return bf(scaled * jax.nn.silu(output_gate_logits.astype(jnp.float32)))


def rms_scale(layer_state, feed_norm_scale):
    widened = layer_state.astype(jnp.float32)
    return (
        widened
        * lax.rsqrt(jnp.mean(widened * widened, axis=-1, keepdims=True) + EPSILON)
        * feed_norm_scale
    ).astype(jnp.bfloat16)


def conv_gate(padded, tap_rows):
    length = padded.shape[0] - 2
    mixed_rows = (
        tap_rows[0] * padded[0:length]
        + tap_rows[1] * padded[1 : length + 1]
        + tap_rows[2] * padded[2 : length + 2]
    )
    half_width = mixed_rows.shape[1] // 2
    return (jax.nn.silu(mixed_rows[:, :half_width]) * mixed_rows[:, half_width:]).astype(
        jnp.bfloat16
    )


def ring_order(mesh):
    count = mesh.shape["sp"]
    places = [getattr(d, "coords", None) for d in mesh.devices.reshape(count, -1)[:, 0]]
    if any(p is None for p in places):
        return list(range(count))
    at = {(p[2], p[1]): index for index, p in enumerate(places)}
    tall = 1 + max(z for z, _ in at)
    wide = 1 + max(y for _, y in at)
    if len(at) != count or tall * wide != count or tall % 2 or wide < 2:
        return list(range(count))
    walk = []
    for z in range(tall):
        ys = range(1, wide) if z % 2 == 0 else range(wide - 1, 0, -1)
        walk += [(z, y) for y in ys]
    walk += [(z, 0) for z in range(tall - 1, -1, -1)]
    return [at[p] for p in walk]


def ring_gather(block, order, step_sign):
    count = len(order)
    pairs = [(order[p], order[(p + step_sign) % count]) for p in range(count)]
    position = [order.index(index) for index in range(count)]
    me = lax.axis_index("sp")
    arrived = [(block, me)]
    for step in range(1, count):
        block = lax.ppermute(block, "sp", pairs)
        owners = [order[(position[index] - step_sign * step) % count] for index in range(count)]
        arrived.append((block, jnp.array(owners, jnp.int32)[me]))
    return arrived


def assemble(arrived, axis):
    block = arrived[0][0]
    shape = list(block.shape)
    extent = shape[axis]
    shape[axis] *= len(arrived)
    whole = jnp.zeros(shape, block.dtype)
    for piece, owner in arrived:
        whole = lax.dynamic_update_slice_in_dim(whole, piece, owner * extent, axis)
    return whole


def entering_states(forward, backward):
    count, me = lax.axis_size("sp"), lax.axis_index("sp")
    received = {}
    for k in range(1, count):
        outgoing = jnp.where(me + k < count, forward, backward)
        received[k] = lax.ppermute(outgoing, "sp", [(p, (p + k) % count) for p in range(count)])
    width = forward.shape[2]
    totals = []
    for ks, later in ((range(1, count), False), (range(count - 1, 0, -1), True)):
        total = jnp.zeros(forward[:, :width].shape, jnp.float32)
        scale = jnp.ones((forward.shape[0], width), jnp.float32)
        for k in ks:
            used = (me - k < 0) if later else (me - k >= 0)
            state = received[k][:, :width].astype(jnp.float32)
            total = total + jnp.where(used, scale, 0.0)[:, :, None] * state
            scale = scale * received[k][:, width].astype(jnp.float32)
        totals.append(total)
    return totals


def on_device(
    order,
    residual,
    query_logits,
    value_written,
    output_gate_logits,
    forget_logits,
    forget_slack,
    spike_log_decay,
    head_norm_scale,
    recurrence_output_matrix,
    feed_norm_scale,
    gate_matrix,
    up_matrix,
    position_filter_taps,
    down_matrix,
):
    halves = down_matrix.shape[0] // 2
    gate_all = assemble(ring_gather(gate_matrix, order, 1), 0)
    up_all = assemble(ring_gather(up_matrix, order, -1), 0)
    down_parts = (
        assemble(ring_gather(down_matrix[:halves], order, 1), 1),
        assemble(ring_gather(down_matrix[halves:], order, -1), 1),
    )
    width = head_norm_scale.shape[0]
    length, columns = query_logits.shape
    place = jnp.arange(length)
    lower = (place[:, None] >= place[None, :]).astype(jnp.float32)
    upper = lower.T
    spike_rows = jnp.stack(
        [
            jnp.dot(spike_log_decay, upper, precision=PRECISE),
            jnp.dot(spike_log_decay, lower, precision=PRECISE),
        ]
    )
    within, states, entering, decays = [], [], [], []
    for head in range(columns // width):
        cut = slice(head * width, (head + 1) * width)
        queries = jax.nn.silu(query_logits[:, cut].astype(jnp.float32))
        pieces = [
          direction(
              queries,
              forget_logits[way][:, cut].astype(jnp.float32),
              forget_slack[way : way + 1, cut],
              (lower, upper)[way],
              spike_rows[way, head][:, None],
              spike_rows[way, head][None, :],
              (-1, 0)[way],
          )
          for way in range(2)
        ]
        within.append(mm(pieces[0][0] + pieces[1][0], value_written[:, cut]))
        states.append([bf(mm(p[1], value_written[:, cut], ((0,), (0,)))) for p in pieces])
        entering.append(bf(jnp.concatenate([p[2] for p in pieces], axis=1)))
        decays.append([p[3][0] for p in pieces])
    carried = []
    for way in range(2):
        state = jnp.stack([pair[way] for pair in states])
        decay = bf(jnp.exp(jnp.stack([pair[way] for pair in decays])))
        rows = jnp.broadcast_to(decay[:, None, :], (decay.shape[0], 16, width))
        carried.append(jnp.concatenate([state, rows], axis=1))
    enters = entering_states(*carried)
    gated = []
    for head in range(columns // width):
        cut = slice(head * width, (head + 1) * width)
        state = jnp.concatenate([enters[0][head], enters[1][head]], axis=0)
        summed = within[head] + mm(entering[head], state)
        gated.append(gate_head(summed, head_norm_scale, output_gate_logits[:, cut]))
    gated_heads = jnp.concatenate(gated, axis=1)
    regrouped = lax.all_to_all(gated_heads, "tp", split_axis=0, concat_axis=1, tiled=True)
    branch = jnp.dot(regrouped, recurrence_output_matrix, preferred_element_type=jnp.float32)
    layer_state = (residual.astype(jnp.float32) + branch).astype(jnp.bfloat16)
    normed = rms_scale(layer_state, feed_norm_scale)
    half = normed.shape[1] // 2
    rest = lax.all_gather(normed[:, half:], "tp", axis=0, tiled=True)
    row_piece = jnp.concatenate(
        [
            lax.all_gather(normed[:, :half], "tp", axis=0, tiled=True),
            rest,
        ],
        axis=1,
    )
    gate_part = jnp.dot(row_piece, gate_all, preferred_element_type=jnp.float32)
    up_part = jnp.dot(row_piece, up_all, preferred_element_type=jnp.float32)
    projected = jnp.concatenate([gate_part, up_part], axis=1).astype(jnp.bfloat16)
    padded = extended(projected, (("sp", 0),), 1)
    tap_rows = jnp.concatenate([position_filter_taps[0], position_filter_taps[1]], axis=1)
    hidden = conv_gate(padded, tap_rows)
    partial = jnp.dot(
        hidden[:, :halves], down_parts[0], preferred_element_type=jnp.float32
    ) + jnp.dot(hidden[:, halves:], down_parts[1], preferred_element_type=jnp.float32)
    groups = lax.axis_size("tp")
    sent = bf(partial).reshape(groups, -1, partial.shape[1])
    channel_out = jnp.sum(
        lax.all_to_all(sent, "tp", split_axis=0, concat_axis=0).astype(jnp.float32), axis=0
    )
    return (layer_state.astype(jnp.float32) + channel_out).astype(jnp.bfloat16)


def solution(mesh):
    placed = (
        P(("sp", "tp"), None),
        P("sp", "tp"),
        P("sp", "tp"),
        P("sp", "tp"),
        P(None, "sp", "tp"),
        P(None, "tp"),
        P("tp", "sp"),
        P(),
        P(),
        P(),
        P("sp", "tp"),
        P("sp", "tp"),
        P(None, None, "tp"),
        P("tp", "sp"),
    )
    def device_step(*args):
        return on_device(ring_order(mesh), *args)

    return jax.shard_map(
        device_step,
        mesh=mesh,
        in_specs=placed,
        out_specs=P(("sp", "tp"), None),
        check_vma=False,
    )
```
